32 devices in a mesh: grp: 2 (over y), sp: 4 (over z), dp: 4 (over x, core).
Axes of the slice: x: 2, y: 2, z: 4, core: 2. Of those that a mesh axis runs over, the one named last changes fastest.
Arguments:
- queries: bfloat16 [8, 512, 16, 192], P(('grp', 'dp'), 'sp'), parts along dimension 0, may hold values from -41 to 41
- kv_latent: bfloat16 [8, 512, 512], P(('grp', 'dp'), 'sp'), parts along dimension 0, may hold values from -6 to 6
- rope_key: bfloat16 [8, 512, 64], P(('grp', 'dp'), 'sp'), parts along dimension 0, may hold values from -5.1 to 5.1
- kv_gain: float32 [512], replicated, may hold values from 0.1 to 1.9
- kv_weight: bfloat16 [512, 4096], P('dp', 'sp'), may hold values from -0.25 to 0.25
- out_weight: bfloat16 [2048, 2048], P(None, 'dp'), may hold values from -1 to 1
Outputs:
- mixed: bfloat16 [8, 512, 2048], P(('grp', 'dp'), 'sp'), parts along dimension 0
The draws below stay inside these ranges and needn't reach their ends.
There are 2 independent parts, one for each index of `grp`. The reference program is written for one: setup_inputs(seed, part) draws one part's arguments, and reference() takes and returns one part's arrays. A program takes and returns all parts, laid end to end along the dimension named above; an argument that names none is the same for every part. Nothing has to cross between parts.
All inputs are finite; a program needn't handle non-finite values.
Results may differ from the reference program's by a relative error of at most 0.0075.
Values may be sent and summed in bfloat16 or wider, within the bound.
A program may use at most 64 MiB of HBM per device.

```python
import jax
import jax.numpy as jnp
from jax import lax

D = 2048
H = 16
KL = 512
NOPE = 128
ROPE = 64
VD = 128
LEN = 512
SEQS = 4


def paired_draw(key):
    base = jax.random.fold_in(key, 41)
    first_key, second_key = jax.random.split(base)
    query_shape = (SEQS, LEN, H, NOPE + ROPE)
    shared = jnp.clip(jax.random.normal(first_key, (SEQS, LEN, ROPE), jnp.float32), -5.0, 5.0)
    query = jnp.clip(jax.random.normal(second_key, query_shape, jnp.float32), -5.0, 5.0)
    return (query, shared)


def draw_queries(key, part):
    return paired_draw(key)[0].astype(jnp.bfloat16)


def draw_rope_key(key, part):
    return paired_draw(key)[1].astype(jnp.bfloat16)


def levels(stream_key, shape, cuts, smallest, high):
    level, own = 1.0, jax.random.fold_in(stream_key, 6)
    for position, parts in cuts:
        draws = jnp.exp(jax.random.uniform(jax.random.fold_in(own, position), (parts,), jnp.float32, smallest / len(cuts), high / len(cuts)))
        level = level * jnp.repeat(draws, shape[position] // parts).reshape([-1 if axis == position else 1 for axis in range(len(shape))])
    return level


def scatter_about(own_key, shape, scale, bound, cuts=(), kind=jnp.bfloat16):
    gain = levels(own_key, shape, cuts, -0.22, 0.18) if cuts else 1.0
    values = jax.random.normal(own_key, shape, jnp.float32) * scale * gain
    return jnp.minimum(jnp.maximum(values, -bound), bound).astype(kind)


def setup_inputs(seed: int = 0, part: int = 0) -> dict:
    seeds = jax.random.split(jax.random.key(seed), 7)
    part_splits = jax.random.split(jax.random.fold_in(seeds[6], part), 7)
    return {
        "queries": draw_queries(jax.random.fold_in(jax.random.fold_in(seeds[6], part), 71), part),
        "kv_latent": scatter_about(part_splits[1], (SEQS, LEN, KL), 1.0, 6.0, ((0, 4), (1, 4))),
        "rope_key": draw_rope_key(jax.random.fold_in(jax.random.fold_in(seeds[6], part), 71), part),
        "kv_gain": jnp.clip(1.0 + 0.18 * jax.random.normal(seeds[3], (KL,), jnp.float32), 0.1, 1.9),
        "kv_weight": scatter_about(seeds[4], (KL, H * (NOPE + VD)), KL ** -0.5, 0.25, ((0, 4), (1, 4))),
        "out_weight": scatter_about(seeds[5], (H * VD, D), 32 ** -0.5, 1.0, ((1, 4),)),
    }


def rotate(values, positions):
    half = values.shape[-1] // 2
    inverse = jnp.power(10000.0, -jnp.arange(half, dtype=jnp.float32) * 2.0 / values.shape[-1])
    angle = positions.astype(jnp.float32)[..., None] * inverse
    first = values[..., :half].astype(jnp.float32)
    second = values[..., half:].astype(jnp.float32)
    cosine = jnp.cos(angle)
    sine = jnp.sin(angle)
    return jnp.concatenate([first * cosine - second * sine, first * sine + second * cosine], axis=-1)

def attend(query_rot, key_value, key_rot):
    length, heads = (query_rot.shape[0], query_rot.shape[1])
    nope = query_rot.shape[2] - key_rot.shape[1]
    scale = query_rot.shape[2] ** (-0.5)
    content = key_value[:, :, :nope]
    values = key_value[:, :, nope:].astype(jnp.float32)
    shared = jnp.broadcast_to(key_rot[:, None, :], (length, heads, key_rot.shape[1]))
    keys = jnp.concatenate([content, shared], axis=-1).astype(jnp.float32)
    block = min(512, length)
    blocks = query_rot.reshape(length // block, block, heads, query_rot.shape[2])
    key_pos = jnp.arange(length, dtype=jnp.int32)

    def one_block(item):
        query_block, index = item
        scores = jnp.einsum('qhd,khd->hqk', query_block.astype(jnp.float32), keys) * scale
        query_pos = index * block + jnp.arange(block, dtype=jnp.int32)
        kept = query_pos[:, None] >= key_pos[None, :]
        scores = jnp.where(kept[None], scores, -jnp.inf)
        top = lax.optimization_barrier(jnp.max(scores, axis=-1, keepdims=True))
        expo = jnp.exp(scores - top)
        probs = (expo / lax.optimization_barrier(jnp.sum(expo, axis=-1, keepdims=True))).astype(jnp.bfloat16)
        return jnp.einsum('hqk,khd->qhd', probs.astype(jnp.float32), values).astype(jnp.bfloat16)
    result = lax.map(one_block, (blocks, jnp.arange(length // block, dtype=jnp.int32)))
    return result.reshape(length, heads, values.shape[2])

def reference(queries, kv_latent, rope_key, kv_gain, kv_weight, out_weight):
    positions = jnp.arange(LEN, dtype=jnp.int32)

    def one_sequence(item):
        query, latent, shared = item
        latent32 = latent.astype(jnp.float32)
        latent_n = (latent32 * lax.rsqrt(lax.optimization_barrier(jnp.mean(latent32 * latent32, axis=-1, keepdims=True)) + 1e-06) * kv_gain).astype(jnp.bfloat16)
        key_value = jnp.dot(latent_n, kv_weight, preferred_element_type=jnp.float32).astype(jnp.bfloat16)
        key_value = key_value.reshape(LEN, H, NOPE + VD)
        key_rot = rotate(shared, positions).astype(jnp.bfloat16)
        turned = rotate(query[:, :, NOPE:], positions[:, None])
        query_rot = jnp.concatenate([query[:, :, :NOPE].astype(jnp.float32), turned], axis=-1).astype(jnp.bfloat16)
        attended = attend(query_rot, key_value, key_rot).reshape(LEN, H * VD)
        return jnp.dot(attended, out_weight, preferred_element_type=jnp.float32).astype(jnp.bfloat16)
    return lax.map(one_sequence, (queries, kv_latent, rope_key))
```

```python
import functools

import jax
import jax.numpy as jnp
from jax import lax
from jax.experimental import pallas as pl
from jax.experimental.pallas import tpu as pltpu
from jax.sharding import PartitionSpec as P

NOPE = 128
VD = 128
LANES = 128
CORES = 2
CHUNKS = 8
MESH = pl.DeviceIdType.MESH


def rotate(values, positions):
    half = values.shape[-1] // 2
    inverse = jnp.power(10000.0, -jnp.arange(half, dtype=jnp.float32) * 2.0 / values.shape[-1])
    angle = positions.astype(jnp.float32)[..., None] * inverse
    first = values[..., :half].astype(jnp.float32)
    second = values[..., half:].astype(jnp.float32)
    cosine = jnp.cos(angle)
    sine = jnp.sin(angle)
    return jnp.concatenate(
        [first * cosine - second * sine, first * sine + second * cosine], axis=-1
    )


def kernel(
    n, g, nx, hn, rope, scale, chunks,
    q_ref, lat_ref, kvw_ref, w_ref, out_ref,
    qbuf, lat, kvw, wfull, kcat, vbuf, attsend, attrecv, acc,
    loc, q_s, q_r, a_s, a_r, lr_s, lr_r, rl_s, rl_r,
    kx_s, kx_r, kc_s, kc_r, wx_s, wx_r, wy_s, wy_r, wc_s, wc_r, wo_s, wo_r,
):
    me = lax.axis_index("sp")
    y = lax.axis_index("grp")
    dp = lax.axis_index("dp")
    x, c = dp // CORES, dp % CORES
    ndp = nx * CORES
    tok = lat_ref.shape[0]
    latw = kvw.shape[0]
    length = n * tok
    krows = kvw_ref.shape[0]
    part = w_ref.shape[0] // g
    crow = part // chunks
    cols = w_ref.shape[1]
    kd = hn * VD
    per_tile = LANES // rope

    def chip(xx, cc):
        return {"dp": xx * CORES + cc}

    partner = chip(x, 1 - c)

    def remote(src, dst, ss, rs, dev):
        return pltpu.make_async_remote_copy(
            src_ref=src, dst_ref=dst, send_sem=ss, recv_sem=rs, device_id=dev, device_id_type=MESH
        )

    own_w = pltpu.make_async_copy(w_ref, wfull.at[dp], loc.at[0])
    own_k = pltpu.make_async_copy(
        kvw_ref, kvw.at[pl.ds(pl.multiple_of(dp * krows, krows), krows)], loc.at[1]
    )
    own_q = pltpu.make_async_copy(q_ref.at[me], qbuf.at[me], loc.at[2])
    own_l = pltpu.make_async_copy(lat_ref, lat.at[me], loc.at[3])
    for copy in (own_k, own_q, own_l, own_w):
        copy.start()

    barrier = pltpu.get_barrier_semaphore()
    for o in range(1, n):
        pl.semaphore_signal(barrier, 1, device_id={"sp": lax.rem(me + o, n)}, device_id_type=MESH)
    for o in range(1, nx):
        pl.semaphore_signal(barrier, 1, device_id=chip(lax.rem(x + o, nx), c), device_id_type=MESH)
    for o in range(1, g):
        pl.semaphore_signal(barrier, 1, device_id={"grp": lax.rem(y + o, g)}, device_id_type=MESH)
    pl.semaphore_signal(barrier, 1, device_id=partner, device_id_type=MESH)
    pl.semaphore_wait(barrier, (n - 1) + (nx - 1) + (g - 1) + 1)

    def to_right(k, src):
        j = me - k
        return remote(src, lat.at[j], lr_s.at[k], lr_r.at[k], {"sp": me + 1})

    def to_left(k, src):
        j = me + k
        return remote(src, lat.at[j], rl_s.at[k], rl_r.at[k], {"sp": me - 1})

    @pl.when(me < n - 1)
    def _():
        to_right(0, lat_ref).start()

    @pl.when(me > 0)
    def _():
        to_left(0, lat_ref).start()

    def kv_rows(d):
        return kvw.at[pl.ds(pl.multiple_of(d * krows, krows), krows)]

    def kv_x(o):
        return remote(kvw_ref, kv_rows(dp), kx_s.at[o - 1], kx_r.at[o - 1], chip(lax.rem(x + o, nx), c))

    def kv_core(o):
        d = lax.rem(x + nx - o, nx) * CORES + c
        src = kvw_ref if o == 0 else kv_rows(d)
        return remote(src, kv_rows(d), kc_s.at[o], kc_r.at[o], partner)

    for o in range(1, nx):
        kv_x(o).start()
    kv_core(0).start()

    def q_copy(o):
        to = lax.rem(me + o, n)
        return remote(q_ref.at[to], qbuf.at[me], q_s.at[o], q_r.at[o], {"sp": to})

    for o in range(1, n):
        q_copy(o).start()

    def w_rows(yy, ch):
        return pl.ds(pl.multiple_of(yy * part + ch * crow, crow), crow)

    def w_x(o, ch):
        rows = w_rows(y, ch)
        return remote(
            w_ref.at[rows], wfull.at[dp, rows], wx_s.at[o - 1, ch], wx_r.at[o - 1, ch],
            chip(lax.rem(x + o, nx), c),
        )

    def w_y(o, p, ch):
        ref = wfull.at[lax.rem(x + nx - o, nx) * CORES + c, w_rows(y, ch)]
        return remote(
            ref, ref, wy_s.at[o - 1, p - 1, ch], wy_r.at[o - 1, p - 1, ch],
            {"grp": lax.rem(y + p, g)},
        )

    def w_c(o, p, ch):
        ref = wfull.at[lax.rem(x + nx - o, nx) * CORES + c, w_rows(lax.rem(y + g - p, g), ch)]
        return remote(ref, ref, wc_s.at[o - 1, p, ch], wc_r.at[o - 1, p, ch], partner)

    for ch in range(chunks):
        for o in range(1, nx):
            w_x(o, ch).start()
    w_own = remote(w_ref, wfull.at[dp], wo_s, wo_r, partner)
    w_own.start()

    own_l.wait()
    for k in range(1, n):
        @pl.when(me - k >= 0)
        def _():
            to_right(k - 1, lat_ref).wait_recv()

            @pl.when(me < n - 1)
            def _():
                to_right(k, lat.at[me - k]).start()

        @pl.when(me + k < n)
        def _():
            to_left(k - 1, lat_ref).wait_recv()

            @pl.when(me > 0)
            def _():
                to_left(k, lat.at[me + k]).start()

    for o in range(1, nx):
        kv_x(o).wait_recv()
        kv_core(o).start()
    own_k.wait()
    for o in range(nx):
        kv_core(o).wait_recv()

    lane = lax.broadcasted_iota(jnp.int32, (tok, LANES), 1)

    @pl.loop(0, n)
    def _(j):
        rows = pl.ds(pl.multiple_of(j * tok, tok), tok)
        shared = lat[j, :, latw:].astype(jnp.float32)
        spread = [
            jnp.where(lane // rope == i, shared, 0.0).astype(jnp.bfloat16) for i in range(per_tile)
        ]
        block = lat[j, :, :latw]
        for h in range(hn):
            wide = NOPE + VD
            both = jnp.dot(
                block, kvw[:, h * wide : (h + 1) * wide], preferred_element_type=jnp.float32
            ).astype(jnp.bfloat16)
            kcat[h, rows, :NOPE] = both[:, :NOPE]
            kcat[h, rows, NOPE:] = spread[h % per_tile]
            vbuf[h, rows, :] = both[:, NOPE:]

    def pass_x(ch):
        for o in range(1, nx):
            w_x(o, ch).wait_recv()
            for p in range(1, g):
                w_y(o, p, ch).start()
            w_c(o, 0, ch).start()

    def pass_y(ch):
        for o in range(1, nx):
            for p in range(1, g):
                w_y(o, p, ch).wait_recv()
                w_c(o, p, ch).start()

    def attention(j):
        col = lax.broadcasted_iota(jnp.int32, (tok, length), 1)
        row = lax.broadcasted_iota(jnp.int32, (tok, length), 0)
        kept = col - row <= j * tok
        for h in range(hn):
            query = jnp.concatenate([qbuf[j, h], qbuf[j, hn + h // per_tile]], axis=-1)
            s = lax.dot_general(
                query, kcat[h], (((1,), (1,)), ((), ())), preferred_element_type=jnp.float32
            ) * scale
            s = jnp.where(kept, s, -jnp.inf)
            top = jnp.max(s, axis=-1, keepdims=True)
            e = jnp.exp(s - top)
            p = (e * (1.0 / jnp.sum(e, axis=-1, keepdims=True))).astype(jnp.bfloat16)
            o = jnp.dot(p, vbuf[h], preferred_element_type=jnp.float32).astype(jnp.bfloat16)
            attsend[j, :, h * VD : (h + 1) * VD] = o

    def a_copy(o):
        to = lax.rem(me + n - o, n)
        return remote(attsend.at[to], attrecv.at[me], a_s.at[o], a_r.at[o], {"sp": to})

    own_q.wait()
    attention(me)
    own_a = pltpu.make_async_copy(attsend.at[me], attrecv.at[me], loc.at[4])
    own_a.start()

    per = -(-chunks // n)
    for b in range(min(per, chunks)):
        pass_x(b)

    @pl.loop(1, n)
    def _(o):
        q_copy(o).wait_recv()
        attention(lax.rem(me + n - o, n))
        a_copy(o).start()
        for b in range(per):
            ch = o * per + b

            @pl.when(ch < chunks)
            def _():
                pass_x(ch)

            @pl.when(ch - per < chunks)
            def _():
                pass_y(ch - per)

    for ch in range(chunks):
        if ch >= (n - 1) * per:
            pass_y(ch)

    own_w.wait()
    w_own.wait_recv()
    for o in range(1, nx):
        for p in range(g):
            for ch in range(chunks):
                w_c(o, p, ch).wait_recv()
    own_a.wait()

    def project(j, first):
        rows = pl.ds(pl.multiple_of(j * kd, kd), kd)
        block = attrecv[j]
        for d in range(ndp):
            part_sum = jnp.dot(block, wfull[d, rows, :], preferred_element_type=jnp.float32)
            if first:
                acc[:, d * cols : (d + 1) * cols] = part_sum
            else:
                acc[:, d * cols : (d + 1) * cols] += part_sum

    project(me, True)

    @pl.loop(1, n)
    def _(o):
        a_copy(o).wait_recv()
        project(lax.rem(me + o, n), False)

    out_ref[...] = acc[...].astype(out_ref.dtype)

    for k in range(n - 1):
        @pl.when((me - k >= 0) & (me < n - 1))
        def _():
            to_right(k, lat_ref).wait_send()

        @pl.when((me + k < n) & (me > 0))
        def _():
            to_left(k, lat_ref).wait_send()
    for o in range(1, n):
        q_copy(o).wait_send()
        a_copy(o).wait_send()
    w_own.wait_send()
    for o in range(nx):
        kv_core(o).wait_send()
    for o in range(1, nx):
        kv_x(o).wait_send()
        for ch in range(chunks):
            w_x(o, ch).wait_send()
            for p in range(1, g):
                w_y(o, p, ch).wait_send()
            for p in range(g):
                w_c(o, p, ch).wait_send()


def body(sizes, queries, kv_latent, rope_key, kv_gain, kv_weight, out_weight):
    g, n, dp = sizes
    nx = dp // CORES
    tok, heads, width = queries.shape[1:]
    rope = width - NOPE
    hn = heads // n
    latw = kv_latent.shape[2]
    positions = lax.axis_index("sp") * tok + jnp.arange(tok, dtype=jnp.int32)
    latent32 = kv_latent[0].astype(jnp.float32)
    latent_n = (
        latent32
        * lax.rsqrt(jnp.mean(latent32 * latent32, axis=-1, keepdims=True) + 1e-06)
        * kv_gain
    ).astype(jnp.bfloat16)
    key_rot = rotate(rope_key[0], positions).astype(jnp.bfloat16)
    packed = jnp.concatenate([latent_n] + [key_rot] * (LANES // rope), axis=1)
    turned = rotate(queries[0, :, :, NOPE:], positions[:, None]).astype(jnp.bfloat16)
    content = queries[0, :, :, :NOPE].reshape(tok, n, hn, NOPE).transpose(1, 2, 0, 3)
    tiles = -(-hn * rope // LANES)
    turned = turned.reshape(tok, n, hn * rope)
    turned = jnp.pad(turned, ((0, 0), (0, 0), (0, tiles * LANES - hn * rope)))
    turned = turned.reshape(tok, n, tiles, LANES).transpose(1, 2, 0, 3)
    q = jnp.concatenate([content, turned], axis=1)

    d_in, cols = out_weight.shape
    part = d_in // g
    chunks = CHUNKS
    kcols = kv_weight.shape[1]
    dma = pltpu.SemaphoreType.DMA
    bf = jnp.bfloat16
    xn = max(nx - 1, 1)
    gn = max(g - 1, 1)
    vmem = pl.BlockSpec(memory_space=pltpu.VMEM)
    out = pl.pallas_call(
        functools.partial(kernel, n, g, nx, hn, rope, width**-0.5, chunks),
        out_shape=jax.ShapeDtypeStruct((tok, cols * dp), bf),
        in_specs=[vmem, vmem, vmem, pl.BlockSpec(memory_space=pltpu.HBM)],
        out_specs=vmem,
        scratch_shapes=[
            pltpu.VMEM((n, hn + tiles, tok, LANES), bf),
            pltpu.VMEM((n, tok, latw + LANES), bf),
            pltpu.VMEM((kv_weight.shape[0] * dp, kcols), bf),
            pltpu.VMEM((dp, d_in, cols), bf),
            pltpu.VMEM((hn, n * tok, NOPE + LANES), bf),
            pltpu.VMEM((hn, n * tok, VD), bf),
            pltpu.VMEM((n, tok, hn * VD), bf),
            pltpu.VMEM((n, tok, hn * VD), bf),
            pltpu.VMEM((tok, cols * dp), jnp.float32),
            dma((5,)),
            dma((n,)), dma((n,)), dma((n,)), dma((n,)),
            dma((n,)), dma((n,)), dma((n,)), dma((n,)),
            dma((xn,)), dma((xn,)), dma((nx,)), dma((nx,)),
            dma((xn, chunks)), dma((xn, chunks)),
            dma((xn, gn, chunks)), dma((xn, gn, chunks)),
            dma((xn, g, chunks)), dma((xn, g, chunks)),
            dma(()), dma(()),
        ],
        compiler_params=pltpu.CompilerParams(
            collective_id=0, has_side_effects=True, vmem_limit_bytes=56 * 1024 * 1024
        ),
    )(q, packed, kv_weight, out_weight)
    return out[None]


def solution(mesh):
    sizes = (mesh.shape["grp"], mesh.shape["sp"], mesh.shape["dp"])
    return jax.shard_map(
        functools.partial(body, sizes),
        mesh=mesh,
        in_specs=(
            P(("grp", "dp"), "sp", None, None),
            P(("grp", "dp"), "sp", None),
            P(("grp", "dp"), "sp", None),
            P(),
            P("dp", "sp"),
            P(None, "dp"),
        ),
        out_specs=P(("grp", "dp"), "sp", None),
        check_vma=False,
    )
```

```python
import functools
import math

import jax
import jax.numpy as jnp
import numpy as np
from jax import lax
from jax.experimental import pallas as pl
from jax.experimental.pallas import tpu as pltpu
from jax.sharding import PartitionSpec as P

NOPE = 128
VD = 128
LANES = 128
CORES = 2
CHUNKS = 8
MESH = pl.DeviceIdType.MESH


VARIANTS = 4


def rotation_table(length, rope):
    half = rope // 2
    inverse = np.power(10000.0, -np.arange(half) * 2.0 / rope).astype(np.float32)
    angle = inverse[:, None] * np.arange(length, dtype=np.float32)[None, :]
    return np.stack([np.cos(angle), np.sin(angle)]).astype(np.float32)


def kernel(
    n, g, nx, hn, rope, scale, chunks,
    q_ref, latent_ref, key_ref, gain_ref, table_ref, kvw_ref, w_ref, out_ref,
    qbuf, lat, kvw, wfull, kcat, vbuf, attsend, attrecv, acc,
    loc, q_s, q_r, a_s, a_r, lr_s, lr_r, rl_s, rl_r,
    kx_s, kx_r, kc_s, kc_r, wx_s, wx_r, wy_s, wy_r, wc_s, wc_r, wo_s, wo_r,
):
    me = lax.axis_index("sp")
    y = lax.axis_index("grp")
    dp = lax.axis_index("dp")
    x, c = dp // CORES, dp % CORES
    ndp = nx * CORES
    tok = latent_ref.shape[0]
    half = rope // 2
    lat_ref = lat.at[me]
    latw = kvw.shape[0]
    length = n * tok
    krows = kvw_ref.shape[0]
    part = w_ref.shape[0] // g
    crow = part // chunks
    cols = w_ref.shape[1]
    kd = hn * VD

    def xor(a, b):
        total, bit = 0, 1
        while bit < n:
            total = total + bit * lax.rem(lax.div(a, bit) + lax.div(jnp.int32(b), bit), 2)
            bit *= 2
        return total

    paired = n & (n - 1) == 0

    def target(o):
        return xor(me, o) if paired else lax.rem(me + o, n)

    def source(o):
        return xor(me, o) if paired else lax.rem(me + n - o, n)

    def turned(values, j):
        span = pl.ds(pl.multiple_of(j * tok, tok), tok)
        cosine, sine = table_ref[0, :, span], table_ref[1, :, span]
        first, second = values[:half].astype(jnp.float32), values[half:].astype(jnp.float32)
        return first * cosine - second * sine, first * sine + second * cosine

    def chip(xx, cc):
        return {"dp": xx * CORES + cc}

    partner = chip(x, 1 - c)

    def remote(src, dst, ss, rs, dev):
        return pltpu.make_async_remote_copy(
            src_ref=src, dst_ref=dst, send_sem=ss, recv_sem=rs, device_id=dev, device_id_type=MESH
        )

    own_w = pltpu.make_async_copy(w_ref, wfull.at[dp], loc.at[0])
    own_k = pltpu.make_async_copy(
        kvw_ref, kvw.at[pl.ds(pl.multiple_of(dp * krows, krows), krows)], loc.at[1]
    )
    own_q = pltpu.make_async_copy(q_ref.at[pl.ds(me * hn, hn)], qbuf.at[me], loc.at[2])
    for copy in (own_k, own_q, own_w):
        copy.start()

    barrier = pltpu.get_barrier_semaphore()
    for o in range(1, n):
        pl.semaphore_signal(barrier, 1, device_id={"sp": lax.rem(me + o, n)}, device_id_type=MESH)
    for o in range(1, nx):
        pl.semaphore_signal(barrier, 1, device_id=chip(lax.rem(x + o, nx), c), device_id_type=MESH)
    for o in range(1, g):
        pl.semaphore_signal(barrier, 1, device_id={"grp": lax.rem(y + o, g)}, device_id_type=MESH)
    pl.semaphore_signal(barrier, 1, device_id=partner, device_id_type=MESH)

    latent = latent_ref[...].astype(jnp.float32)
    square = jnp.mean(latent * latent, axis=-1, keepdims=True)
    lat[me, :, :latw] = (latent * lax.rsqrt(square + 1e-06) * gain_ref[...]).astype(jnp.bfloat16)
    first, second = turned(key_ref[...], me)
    rest = jnp.zeros((LANES - rope, tok), jnp.float32)
    lat[me, :, latw:] = jnp.concatenate([first, second, rest], axis=0).T.astype(jnp.bfloat16)

    pl.semaphore_wait(barrier, (n - 1) + (nx - 1) + (g - 1) + 1)

    def to_right(k, src):
        j = me - k
        return remote(src, lat.at[j], lr_s.at[k], lr_r.at[k], {"sp": me + 1})

    def to_left(k, src):
        j = me + k
        return remote(src, lat.at[j], rl_s.at[k], rl_r.at[k], {"sp": me - 1})

    @pl.when(me < n - 1)
    def _():
        to_right(0, lat_ref).start()

    @pl.when(me > 0)
    def _():
        to_left(0, lat_ref).start()

    def kv_rows(d):
        return kvw.at[pl.ds(pl.multiple_of(d * krows, krows), krows)]

    def kv_x(o):
        return remote(kvw_ref, kv_rows(dp), kx_s.at[o - 1], kx_r.at[o - 1], chip(lax.rem(x + o, nx), c))

    def kv_core(o):
        d = lax.rem(x + nx - o, nx) * CORES + c
        src = kvw_ref if o == 0 else kv_rows(d)
        return remote(src, kv_rows(d), kc_s.at[o], kc_r.at[o], partner)

    for o in range(1, nx):
        kv_x(o).start()
    kv_core(0).start()

    def q_copy(o):
        to = target(o)
        return remote(q_ref.at[pl.ds(to * hn, hn)], qbuf.at[me], q_s.at[o], q_r.at[o], {"sp": to})

    for o in range(1, n):
        q_copy(o).start()

    def w_rows(yy, ch):
        return pl.ds(pl.multiple_of(yy * part + ch * crow, crow), crow)

    def w_x(o, ch):
        rows = w_rows(y, ch)
        return remote(
            w_ref.at[rows], wfull.at[dp, rows], wx_s.at[o - 1, ch], wx_r.at[o - 1, ch],
            chip(lax.rem(x + o, nx), c),
        )

    def w_y(o, p, ch):
        ref = wfull.at[lax.rem(x + nx - o, nx) * CORES + c, w_rows(y, ch)]
        return remote(
            ref, ref, wy_s.at[o - 1, p - 1, ch], wy_r.at[o - 1, p - 1, ch],
            {"grp": lax.rem(y + p, g)},
        )

    def w_c(o, p, ch):
        ref = wfull.at[lax.rem(x + nx - o, nx) * CORES + c, w_rows(lax.rem(y + g - p, g), ch)]
        return remote(ref, ref, wc_s.at[o - 1, p, ch], wc_r.at[o - 1, p, ch], partner)

    for ch in range(chunks):
        for o in range(1, nx):
            w_x(o, ch).start()
    w_own = remote(w_ref, wfull.at[dp], wo_s, wo_r, partner)
    w_own.start()

    for k in range(1, n):
        @pl.when(me - k >= 0)
        def _():
            to_right(k - 1, lat_ref).wait_recv()

            @pl.when(me < n - 1)
            def _():
                to_right(k, lat.at[me - k]).start()

        @pl.when(me + k < n)
        def _():
            to_left(k - 1, lat_ref).wait_recv()

            @pl.when(me > 0)
            def _():
                to_left(k, lat.at[me + k]).start()

    for o in range(1, nx):
        kv_x(o).wait_recv()
        kv_core(o).start()
    own_k.wait()
    for o in range(nx):
        kv_core(o).wait_recv()

    @pl.loop(0, n)
    def _(j):
        rows = pl.ds(pl.multiple_of(j * tok, tok), tok)
        block = lat[j, :, :latw]
        shared = lat[j, :, latw:]
        for h in range(hn):
            wide = NOPE + VD
            both = jnp.dot(
                block, kvw[:, h * wide : (h + 1) * wide], preferred_element_type=jnp.float32
            )
            kcat[h, rows, :NOPE] = both[:, :NOPE].astype(jnp.bfloat16)
            kcat[h, rows, NOPE:] = shared
            vbuf[h, :, rows] = both[:, NOPE:].T.astype(jnp.bfloat16)

    def pass_x(ch):
        for o in range(1, nx):
            w_x(o, ch).wait_recv()
            for p in range(1, g):
                w_y(o, p, ch).start()
            w_c(o, 0, ch).start()

    def pass_y(ch):
        for o in range(1, nx):
            for p in range(1, g):
                w_y(o, p, ch).wait_recv()
                w_c(o, p, ch).start()

    variants = math.gcd(VARIANTS, n)
    step = length // variants

    def attention_over(j, extent):
        row = lax.broadcasted_iota(jnp.int32, (step, tok), 0)
        col = lax.broadcasted_iota(jnp.int32, (step, tok), 1)
        kept = row - col <= j * tok - (extent - step)
        pad = jnp.zeros((LANES - rope, tok), jnp.bfloat16)
        for h in range(hn):
            first, second = turned(qbuf[j, h, NOPE:, :], j)
            query = jnp.concatenate(
                [qbuf[j, h, :NOPE, :], first.astype(jnp.bfloat16), second.astype(jnp.bfloat16), pad],
                axis=0,
            )
            s = jnp.dot(kcat[h, :extent, :], query, preferred_element_type=jnp.float32)
            last = jnp.where(kept, s[extent - step :], -jnp.inf)
            s = last if extent == step else jnp.concatenate([s[: extent - step], last], axis=0)
            top = jnp.max(s, axis=0, keepdims=True)
            e = jnp.exp2((s - top) * (scale * math.log2(math.e)))
            total = jnp.sum(e, axis=0, keepdims=True)
            o = jnp.dot(vbuf[h, :, :extent], e.astype(jnp.bfloat16), preferred_element_type=jnp.float32)
            attsend[j, :, h * VD : (h + 1) * VD] = (o / total).T.astype(jnp.bfloat16)

    def attention(j):
        for v in range(variants):
            @pl.when(j // (n // variants) == v)
            def _():
                attention_over(j, (v + 1) * step)

    def a_copy(o):
        to = source(o)
        return remote(attsend.at[to], attrecv.at[me], a_s.at[o], a_r.at[o], {"sp": to})

    own_q.wait()
    per = -(-chunks // n)
    for b in range(min(per, chunks)):
        pass_x(b)

    @pl.loop(0, n)
    def _(o):
        @pl.when(o > 0)
        def _():
            q_copy(o).wait_recv()

        attention(source(o))

        @pl.when(o > 0)
        def _():
            a_copy(o).start()

        for b in range(per):
            @pl.when((o + 1) * per + b < chunks)
            def _():
                pass_x((o + 1) * per + b)

            @pl.when(o * per + b < chunks)
            def _():
                pass_y(o * per + b)

    own_w.wait()
    w_own.wait_recv()
    for o in range(1, nx):
        for p in range(g):
            for ch in range(chunks):
                w_c(o, p, ch).wait_recv()

    def project(j, first):
        rows = pl.ds(pl.multiple_of(j * kd, kd), kd)
        block = attsend[me] if first else attrecv[j]
        for d in range(ndp):
            part_sum = jnp.dot(block, wfull[d, rows, :], preferred_element_type=jnp.float32)
            if first:
                acc[:, d * cols : (d + 1) * cols] = part_sum
            else:
                acc[:, d * cols : (d + 1) * cols] += part_sum

    project(me, True)

    @pl.loop(1, n)
    def _(o):
        a_copy(o).wait_recv()
        project(target(o), False)

    out_ref[...] = acc[...].astype(out_ref.dtype)

    for k in range(n - 1):
        @pl.when((me - k >= 0) & (me < n - 1))
        def _():
            to_right(k, lat_ref).wait_send()

        @pl.when((me + k < n) & (me > 0))
        def _():
            to_left(k, lat_ref).wait_send()
    for o in range(1, n):
        q_copy(o).wait_send()
        a_copy(o).wait_send()
    w_own.wait_send()
    for o in range(nx):
        kv_core(o).wait_send()
    for o in range(1, nx):
        kv_x(o).wait_send()
        for ch in range(chunks):
            w_x(o, ch).wait_send()
            for p in range(1, g):
                w_y(o, p, ch).wait_send()
            for p in range(g):
                w_c(o, p, ch).wait_send()


def body(sizes, queries, kv_latent, rope_key, kv_gain, kv_weight, out_weight):
    g, n, dp = sizes
    nx = dp // CORES
    tok, heads, width = queries.shape[1:]
    rope = width - NOPE
    hn = heads // n
    latw = kv_latent.shape[2]
    q = jnp.transpose(queries[0], (1, 2, 0))
    key = jnp.transpose(rope_key[0])
    table = jnp.asarray(rotation_table(n * tok, rope))

    d_in, cols = out_weight.shape
    part = d_in // g
    chunks = CHUNKS
    kcols = kv_weight.shape[1]
    dma = pltpu.SemaphoreType.DMA
    bf = jnp.bfloat16
    xn = max(nx - 1, 1)
    gn = max(g - 1, 1)
    vmem = pl.BlockSpec(memory_space=pltpu.VMEM)
    hbm = pl.BlockSpec(memory_space=pltpu.HBM)
    out = pl.pallas_call(
        functools.partial(kernel, n, g, nx, hn, rope, width**-0.5, chunks),
        out_shape=jax.ShapeDtypeStruct((tok, cols * dp), bf),
        in_specs=[hbm, vmem, vmem, vmem, vmem, hbm, hbm],
        out_specs=vmem,
        scratch_shapes=[
            pltpu.VMEM((n, hn, width, tok), bf),
            pltpu.VMEM((n, tok, latw + LANES), bf),
            pltpu.VMEM((kv_weight.shape[0] * dp, kcols), bf),
            pltpu.VMEM((dp, d_in, cols), bf),
            pltpu.VMEM((hn, n * tok, NOPE + LANES), bf),
            pltpu.VMEM((hn, VD, n * tok), bf),
            pltpu.VMEM((n, tok, hn * VD), bf),
            pltpu.VMEM((n, tok, hn * VD), bf),
            pltpu.VMEM((tok, cols * dp), jnp.float32),
            dma((3,)),
            dma((n,)), dma((n,)), dma((n,)), dma((n,)),
            dma((n,)), dma((n,)), dma((n,)), dma((n,)),
            dma((xn,)), dma((xn,)), dma((nx,)), dma((nx,)),
            dma((xn, chunks)), dma((xn, chunks)),
            dma((xn, gn, chunks)), dma((xn, gn, chunks)),
            dma((xn, g, chunks)), dma((xn, g, chunks)),
            dma(()), dma(()),
        ],
        compiler_params=pltpu.CompilerParams(
            collective_id=0, has_side_effects=True, vmem_limit_bytes=28 * 1024 * 1024
        ),
    )(q, kv_latent[0], key, kv_gain[None], table, kv_weight, out_weight)
    return out[None]


def solution(mesh):
    sizes = (mesh.shape["grp"], mesh.shape["sp"], mesh.shape["dp"])
    return jax.shard_map(
        functools.partial(body, sizes),
        mesh=mesh,
        in_specs=(
            P(("grp", "dp"), "sp", None, None),
            P(("grp", "dp"), "sp", None),
            P(("grp", "dp"), "sp", None),
            P(),
            P("dp", "sp"),
            P(None, "dp"),
        ),
        out_specs=P(("grp", "dp"), "sp", None),
        check_vma=False,
    )
```

```python
import functools
import math

import jax
import jax.numpy as jnp
import numpy as np
from jax import lax
from jax.experimental import pallas as pl
from jax.experimental.pallas import tpu as pltpu
from jax.sharding import PartitionSpec as P

NOPE = 128
VD = 128
LANES = 128
CORES = 2
CHUNKS = 8
LEAD = 3
MESH = pl.DeviceIdType.MESH


VARIANTS = 4


def rotation_table(length, rope):
    half = rope // 2
    inverse = np.power(10000.0, -np.arange(half) * 2.0 / rope).astype(np.float32)
    angle = inverse[:, None] * np.arange(length, dtype=np.float32)[None, :]
    return np.stack([np.cos(angle), np.sin(angle)]).astype(np.float32)


def kernel(
    n, g, nx, hn, rope, scale, chunks,
    q_ref, latent_ref, key_ref, gain_ref, table_ref, kvw_ref, w_ref, out_ref,
    qbuf, lat, kvw, wfull, kcat, vbuf, attsend, attrecv, acc,
    loc, q_s, q_r, a_s, a_r, lr_s, lr_r, rl_s, rl_r,
    kx_s, kx_r, kc_s, kc_r, wx_s, wx_r, wy_s, wy_r, wc_s, wc_r, wo_s, wo_r,
):
    me = lax.axis_index("sp")
    y = lax.axis_index("grp")
    dp = lax.axis_index("dp")
    x, c = dp // CORES, dp % CORES
    ndp = nx * CORES
    tok = latent_ref.shape[0]
    half = rope // 2
    lat_ref = lat.at[me]
    latw = kvw.shape[0]
    length = n * tok
    krows = kvw_ref.shape[0]
    part = w_ref.shape[0] // g
    crow = part // chunks
    cols = w_ref.shape[1]
    kd = hn * VD

    def xor(a, b):
        total, bit = 0, 1
        while bit < n:
            total = total + bit * lax.rem(lax.div(a, bit) + lax.div(jnp.int32(b), bit), 2)
            bit *= 2
        return total

    paired = n & (n - 1) == 0

    def target(o):
        return xor(me, o) if paired else lax.rem(me + o, n)

    def source(o):
        return xor(me, o) if paired else lax.rem(me + n - o, n)

    def turned(values, j):
        span = pl.ds(pl.multiple_of(j * tok, tok), tok)
        cosine, sine = table_ref[0, :, span], table_ref[1, :, span]
        first, second = values[:half].astype(jnp.float32), values[half:].astype(jnp.float32)
        return first * cosine - second * sine, first * sine + second * cosine

    def chip(xx, cc):
        return {"dp": xx * CORES + cc}

    partner = chip(x, 1 - c)

    def remote(src, dst, ss, rs, dev):
        return pltpu.make_async_remote_copy(
            src_ref=src, dst_ref=dst, send_sem=ss, recv_sem=rs, device_id=dev, device_id_type=MESH
        )

    own_w = pltpu.make_async_copy(w_ref, wfull.at[dp], loc.at[0])
    own_k = pltpu.make_async_copy(
        kvw_ref, kvw.at[pl.ds(pl.multiple_of(dp * krows, krows), krows)], loc.at[1]
    )
    own_q = pltpu.make_async_copy(q_ref.at[pl.ds(me * hn, hn)], qbuf.at[me], loc.at[2])
    for copy in (own_k, own_q, own_w):
        copy.start()

    barrier = pltpu.get_barrier_semaphore()
    for o in range(1, n):
        pl.semaphore_signal(barrier, 1, device_id={"sp": lax.rem(me + o, n)}, device_id_type=MESH)
    for o in range(1, nx):
        pl.semaphore_signal(barrier, 1, device_id=chip(lax.rem(x + o, nx), c), device_id_type=MESH)
    for o in range(1, g):
        pl.semaphore_signal(barrier, 1, device_id={"grp": lax.rem(y + o, g)}, device_id_type=MESH)
    pl.semaphore_signal(barrier, 1, device_id=partner, device_id_type=MESH)

    latent = latent_ref[...].astype(jnp.float32)
    square = jnp.mean(latent * latent, axis=-1, keepdims=True)
    lat[me, :, :latw] = (latent * lax.rsqrt(square + 1e-06) * gain_ref[...]).astype(jnp.bfloat16)
    first, second = turned(key_ref[...], me)
    rest = jnp.zeros((LANES - rope, tok), jnp.float32)
    lat[me, :, latw:] = jnp.concatenate([first, second, rest], axis=0).T.astype(jnp.bfloat16)

    pl.semaphore_wait(barrier, (n - 1) + (nx - 1) + (g - 1) + 1)

    def to_right(k, src):
        j = me - k
        return remote(src, lat.at[j], lr_s.at[k], lr_r.at[k], {"sp": me + 1})

    def to_left(k, src):
        j = me + k
        return remote(src, lat.at[j], rl_s.at[k], rl_r.at[k], {"sp": me - 1})

    @pl.when(me < n - 1)
    def _():
        to_right(0, lat_ref).start()

    @pl.when(me > 0)
    def _():
        to_left(0, lat_ref).start()

    def kv_rows(d):
        return kvw.at[pl.ds(pl.multiple_of(d * krows, krows), krows)]

    def kv_x(o):
        return remote(kvw_ref, kv_rows(dp), kx_s.at[o - 1], kx_r.at[o - 1], chip(lax.rem(x + o, nx), c))

    def kv_core(o):
        d = lax.rem(x + nx - o, nx) * CORES + c
        src = kvw_ref if o == 0 else kv_rows(d)
        return remote(src, kv_rows(d), kc_s.at[o], kc_r.at[o], partner)

    for o in range(1, nx):
        kv_x(o).start()
    kv_core(0).start()

    def q_copy(o):
        to = target(o)
        return remote(q_ref.at[pl.ds(to * hn, hn)], qbuf.at[me], q_s.at[o], q_r.at[o], {"sp": to})

    def w_rows(yy, ch):
        return pl.ds(pl.multiple_of(yy * part + ch * crow, crow), crow)

    def w_x(o, ch):
        rows = w_rows(y, ch)
        return remote(
            w_ref.at[rows], wfull.at[dp, rows], wx_s.at[o - 1, ch], wx_r.at[o - 1, ch],
            chip(lax.rem(x + o, nx), c),
        )

    def w_y(o, p, ch):
        ref = wfull.at[lax.rem(x + nx - o, nx) * CORES + c, w_rows(y, ch)]
        return remote(
            ref, ref, wy_s.at[o - 1, p - 1, ch], wy_r.at[o - 1, p - 1, ch],
            {"grp": lax.rem(y + p, g)},
        )

    def w_c(o, p, ch):
        ref = wfull.at[lax.rem(x + nx - o, nx) * CORES + c, w_rows(lax.rem(y + g - p, g), ch)]
        return remote(ref, ref, wc_s.at[o - 1, p, ch], wc_r.at[o - 1, p, ch], partner)

    w_own = remote(w_ref, wfull.at[dp], wo_s, wo_r, partner)
    w_own.start()

    def start_queries():
        for o in range(1, n):
            q_copy(o).start()

    def take_kv():
        for o in range(1, nx):
            kv_x(o).wait_recv()
            kv_core(o).start()
        for ch in range(min(LEAD, chunks)):
            for o in range(1, nx):
                w_x(o, ch).start()

    for k in range(1, n):
        @pl.when(me - k >= 0)
        def _():
            to_right(k - 1, lat_ref).wait_recv()

            @pl.when(me < n - 1)
            def _():
                to_right(k, lat.at[me - k]).start()

        @pl.when(me + k < n)
        def _():
            to_left(k - 1, lat_ref).wait_recv()

            @pl.when(me > 0)
            def _():
                to_left(k, lat.at[me + k]).start()

        if k == n - 1:
            start_queries()
        if k == 1:
            take_kv()

    own_k.wait()
    for o in range(nx):
        kv_core(o).wait_recv()

    @pl.loop(0, n)
    def _(j):
        rows = pl.ds(pl.multiple_of(j * tok, tok), tok)
        block = lat[j, :, :latw]
        shared = lat[j, :, latw:]
        for h in range(hn):
            wide = NOPE + VD
            both = jnp.dot(
                block, kvw[:, h * wide : (h + 1) * wide], preferred_element_type=jnp.float32
            )
            kcat[h, rows, :NOPE] = both[:, :NOPE].astype(jnp.bfloat16)
            kcat[h, rows, NOPE:] = shared
            vbuf[h, :, rows] = both[:, NOPE:].T.astype(jnp.bfloat16)

    def pass_x(ch):
        for o in range(1, nx):
            w_x(o, ch).wait_recv()

            @pl.when(ch + LEAD < chunks)
            def _():
                w_x(o, ch + LEAD).start()

            for p in range(1, g):
                w_y(o, p, ch).start()
            w_c(o, 0, ch).start()

    def pass_y(ch):
        for o in range(1, nx):
            for p in range(1, g):
                w_y(o, p, ch).wait_recv()
                w_c(o, p, ch).start()

    variants = math.gcd(VARIANTS, n)
    step = length // variants

    def attention_over(j, extent):
        row = lax.broadcasted_iota(jnp.int32, (step, tok), 0)
        col = lax.broadcasted_iota(jnp.int32, (step, tok), 1)
        kept = row - col <= j * tok - (extent - step)
        pad = jnp.zeros((LANES - rope, tok), jnp.bfloat16)
        for h in range(hn):
            first, second = turned(qbuf[j, h, NOPE:, :], j)
            query = jnp.concatenate(
                [qbuf[j, h, :NOPE, :], first.astype(jnp.bfloat16), second.astype(jnp.bfloat16), pad],
                axis=0,
            )
            s = jnp.dot(kcat[h, :extent, :], query, preferred_element_type=jnp.float32)
            last = jnp.where(kept, s[extent - step :], -jnp.inf)
            s = last if extent == step else jnp.concatenate([s[: extent - step], last], axis=0)
            top = jnp.max(s, axis=0, keepdims=True)
            e = jnp.exp2((s - top) * (scale * math.log2(math.e)))
            p = (e * (1.0 / jnp.sum(e, axis=0, keepdims=True))).astype(jnp.bfloat16)
            o = jnp.dot(vbuf[h, :, :extent], p, preferred_element_type=jnp.float32)
            attsend[j, :, h * VD : (h + 1) * VD] = o.T.astype(jnp.bfloat16)

    def attention(j):
        for v in range(variants):
            @pl.when(j // (n // variants) == v)
            def _():
                attention_over(j, (v + 1) * step)

    def a_copy(o):
        to = source(o)
        return remote(attsend.at[to], attrecv.at[me], a_s.at[o], a_r.at[o], {"sp": to})

    own_q.wait()
    per = -(-chunks // n)
    for b in range(min(per, chunks)):
        pass_x(b)

    @pl.loop(0, n)
    def _(o):
        @pl.when(o > 0)
        def _():
            q_copy(o).wait_recv()

        attention(source(o))

        @pl.when(o > 0)
        def _():
            a_copy(o).start()

        for b in range(per):
            @pl.when((o + 1) * per + b < chunks)
            def _():
                pass_x((o + 1) * per + b)

            @pl.when(o * per + b < chunks)
            def _():
                pass_y(o * per + b)

    own_w.wait()
    w_own.wait_recv()
    for o in range(1, nx):
        for p in range(g):
            for ch in range(chunks):
                w_c(o, p, ch).wait_recv()

    def project(j, first):
        rows = pl.ds(pl.multiple_of(j * kd, kd), kd)
        block = attsend[me] if first else attrecv[j]
        for d in range(ndp):
            part_sum = jnp.dot(block, wfull[d, rows, :], preferred_element_type=jnp.float32)
            if first:
                acc[:, d * cols : (d + 1) * cols] = part_sum
            else:
                acc[:, d * cols : (d + 1) * cols] += part_sum

    project(me, True)

    @pl.loop(1, n)
    def _(o):
        a_copy(o).wait_recv()
        project(target(o), False)

    out_ref[...] = acc[...].astype(out_ref.dtype)

    for k in range(n - 1):
        @pl.when((me - k >= 0) & (me < n - 1))
        def _():
            to_right(k, lat_ref).wait_send()

        @pl.when((me + k < n) & (me > 0))
        def _():
            to_left(k, lat_ref).wait_send()
    for o in range(1, n):
        q_copy(o).wait_send()
        a_copy(o).wait_send()
    w_own.wait_send()
    for o in range(nx):
        kv_core(o).wait_send()
    for o in range(1, nx):
        kv_x(o).wait_send()
        for ch in range(chunks):
            w_x(o, ch).wait_send()
            for p in range(1, g):
                w_y(o, p, ch).wait_send()
            for p in range(g):
                w_c(o, p, ch).wait_send()


def body(sizes, queries, kv_latent, rope_key, kv_gain, kv_weight, out_weight):
    g, n, dp = sizes
    nx = dp // CORES
    tok, heads, width = queries.shape[1:]
    rope = width - NOPE
    hn = heads // n
    latw = kv_latent.shape[2]
    q = jnp.transpose(queries[0], (1, 2, 0))
    key = jnp.transpose(rope_key[0])
    table = jnp.asarray(rotation_table(n * tok, rope))

    d_in, cols = out_weight.shape
    part = d_in // g
    chunks = CHUNKS
    kcols = kv_weight.shape[1]
    dma = pltpu.SemaphoreType.DMA
    bf = jnp.bfloat16
    xn = max(nx - 1, 1)
    gn = max(g - 1, 1)
    vmem = pl.BlockSpec(memory_space=pltpu.VMEM)
    hbm = pl.BlockSpec(memory_space=pltpu.HBM)
    out = pl.pallas_call(
        functools.partial(kernel, n, g, nx, hn, rope, width**-0.5, chunks),
        out_shape=jax.ShapeDtypeStruct((tok, cols * dp), bf),
        in_specs=[hbm, vmem, vmem, vmem, vmem, hbm, hbm],
        out_specs=vmem,
        scratch_shapes=[
            pltpu.VMEM((n, hn, width, tok), bf),
            pltpu.VMEM((n, tok, latw + LANES), bf),
            pltpu.VMEM((kv_weight.shape[0] * dp, kcols), bf),
            pltpu.VMEM((dp, d_in, cols), bf),
            pltpu.VMEM((hn, n * tok, NOPE + LANES), bf),
            pltpu.VMEM((hn, VD, n * tok), bf),
            pltpu.VMEM((n, tok, hn * VD), bf),
            pltpu.VMEM((n, tok, hn * VD), bf),
            pltpu.VMEM((tok, cols * dp), jnp.float32),
            dma((3,)),
            dma((n,)), dma((n,)), dma((n,)), dma((n,)),
            dma((n,)), dma((n,)), dma((n,)), dma((n,)),
            dma((xn,)), dma((xn,)), dma((nx,)), dma((nx,)),
            dma((xn, chunks)), dma((xn, chunks)),
            dma((xn, gn, chunks)), dma((xn, gn, chunks)),
            dma((xn, g, chunks)), dma((xn, g, chunks)),
            dma(()), dma(()),
        ],
        compiler_params=pltpu.CompilerParams(
            collective_id=0, has_side_effects=True, vmem_limit_bytes=28 * 1024 * 1024
        ),
    )(q, kv_latent[0], key, kv_gain[None], table, kv_weight, out_weight)
    return out[None]


def solution(mesh):
    sizes = (mesh.shape["grp"], mesh.shape["sp"], mesh.shape["dp"])
    return jax.shard_map(
        functools.partial(body, sizes),
        mesh=mesh,
        in_specs=(
            P(("grp", "dp"), "sp", None, None),
            P(("grp", "dp"), "sp", None),
            P(("grp", "dp"), "sp", None),
            P(),
            P("dp", "sp"),
            P(None, "dp"),
        ),
        out_specs=P(("grp", "dp"), "sp", None),
        check_vma=False,
    )
```
